32 devices in a mesh: fs: 8 (over z, x), tp: 4 (over y, core).
Axes of the slice: x: 2, y: 2, z: 4, core: 2. Of those that a mesh axis runs over, the one named last changes fastest.
Arguments:
- inputs: bfloat16 [3072, 2048], P('fs'), may hold values from -6 to 6
- queries: bfloat16 [3072, 2048], P('fs', 'tp'), may hold values from -6 to 6
- keys: bfloat16 [3072, 2048], P('fs', 'tp'), may hold values from -6 to 6
- values: bfloat16 [3072, 2048], P('fs', 'tp'), may hold values from -6 to 6
- head_cot: bfloat16 [3072, 2048], P('fs', 'tp'), may hold values from -6 to 6
- mixing: float32 [16], P('tp'), may hold values from 0.3 to 0.8
- head_gain: float32 [128], replicated, may hold values from 0.1 to 1.9
- factors: bfloat16 [2048, 2, 256], P('fs'), may hold values from -0.375 to 0.375
- moments: float32 [256, 2, 2048], P('fs', None, 'tp'), may hold values from -6 to 6
- weights: float32 [2048, 2, 2048], P('fs', None, 'tp'), may hold values from -6 to 6
Outputs:
- step: float32 [2048, 2, 2048], P('fs', None, 'tp')
- new_moments: float32 [256, 2, 2048], P('fs', None, 'tp')
- copies: bfloat16 [2048, 2, 2048], P(None, None, 'tp')
The draws below stay inside these ranges and needn't reach their ends.
All inputs are finite; a program needn't handle non-finite values.
Results may differ from the reference program's by a relative error of at most 0.007.
Values may be sent and summed in bfloat16 or wider, within the bound.
A program may use at most 64 MiB of HBM per device.

```python
import jax
import jax.numpy as jnp
from jax import lax

D = 2048
HEADS = 16
HEAD_DIM = 64
RANK = 256
TOK_DEV = 384
HV = 2048
TOKENS = 3072


def pair_draw(key):
    shape = (TOKENS, HV)
    first_key, second_key = jax.random.split(jax.random.fold_in(key, 17), 2)
    query_vals = jnp.clip(jax.random.normal(first_key, shape, jnp.float32) * 1.3, -6.0, 6.0)
    key_vals = jnp.clip(jax.random.normal(second_key, shape, jnp.float32) * 1.3, -6.0, 6.0)
    return (query_vals, key_vals)


def draw_queries(key, part):
    return pair_draw(key)[0].astype(jnp.bfloat16)


def draw_keys(key, part):
    return pair_draw(key)[1].astype(jnp.bfloat16)


def steps_of(key, shape, cuts, low, largest):
    gain = 1.0
    for position, shards_of in cuts:
        heights = jax.random.uniform(jax.random.fold_in(jax.random.fold_in(key, 6), position), (shards_of,), jnp.float32, low / len(cuts), largest / len(cuts))
        gain = gain * jnp.repeat(jnp.exp(heights), shape[position] // shards_of).reshape((-1,) + (1,) * (len(shape) - 1 - position))
    return gain


def bell_draw(stream_key, shape, deviation, reach, cuts=(), kind=jnp.bfloat16):
    result = deviation * jax.random.normal(stream_key, shape, jnp.float32)
    if cuts:
        result = result * steps_of(stream_key, shape, cuts, -0.22, 0.18)
    return jnp.clip(result, -reach, reach).astype(kind)


def setup_inputs(seed: int = 0) -> dict:
    splits = jax.random.split(jax.random.key(seed), 11)
    return {
        "inputs": bell_draw(splits[0], (TOKENS, D), 1.0, 6.0, ((0, 8),)),
        "queries": draw_queries(jax.random.fold_in(splits[10], 71), 0),
        "keys": draw_keys(jax.random.fold_in(splits[10], 71), 0),
        "values": bell_draw(splits[3], (TOKENS, HV), 1.0, 6.0, ((0, 8), (1, 4))),
        "head_cot": bell_draw(splits[4], (TOKENS, HV), 1.0, 6.0, ((0, 8), (1, 4))),
        "mixing": jnp.clip(0.3 + 0.5 * jax.random.uniform(splits[5], (HEADS,), jnp.float32) ** steps_of(splits[5], (HEADS,), ((0, 4),), -0.2, 0.2), 0.3, 0.8),
        "head_gain": jnp.clip(1.0 + 0.18 * jax.random.normal(splits[6], (2 * HEAD_DIM,), jnp.float32), 0.1, 1.9),
        "factors": bell_draw(splits[7], (D, 2, RANK), RANK ** -0.5, 0.375, ((0, 8),)),
        "moments": bell_draw(splits[8], (RANK, 2, HV), 1.0, 6.0, ((0, 8), (2, 4)), jnp.float32),
        "weights": bell_draw(splits[9], (D, 2, HV), 1.0, 6.0, ((0, 8), (2, 4)), jnp.float32),
    }


EPS = 0.05
BETA = 0.9
RATE_BASE = 0.5

def softmax_rows(scores):
    top = lax.optimization_barrier(jnp.max(scores, axis=-1, keepdims=True))
    expo = jnp.exp(scores - top)
    return expo / lax.optimization_barrier(jnp.sum(expo, axis=-1, keepdims=True))

def head_grads(query, key_rows, value, upstream, weight_mix, head_gain):
    length = query.shape[0]
    head_dim = query.shape[2]
    factor = head_dim ** (-0.5)
    places = jnp.arange(length)
    causal = places[None, :] <= places[:, None]

    def probs(which):
        scores = jnp.dot(query[:, which], key_rows[:, which].T, preferred_element_type=jnp.float32) * factor
        return softmax_rows(jnp.where(causal, scores, -jnp.inf))
    first = probs(0)
    second = probs(1)
    mixed = (first - weight_mix * second).astype(jnp.bfloat16)
    output = jnp.dot(mixed, value, preferred_element_type=jnp.float32)
    inverse = lax.rsqrt(lax.optimization_barrier(jnp.mean(output * output, axis=-1, keepdims=True)) + EPS)
    scaled = head_gain * upstream.astype(jnp.float32)
    d_out = inverse * scaled - output * inverse ** 3 * lax.optimization_barrier(jnp.mean(output * scaled, axis=-1, keepdims=True))
    d_out = d_out.astype(jnp.bfloat16)
    d_value = jnp.dot(mixed.T, d_out, preferred_element_type=jnp.float32).astype(jnp.bfloat16)
    d_mix = jnp.dot(d_out, value.T, preferred_element_type=jnp.float32)
    d_first = (first * (d_mix - lax.optimization_barrier(jnp.sum(first * d_mix, axis=-1, keepdims=True)))).astype(jnp.bfloat16)
    d_second = (-weight_mix * second * (d_mix - lax.optimization_barrier(jnp.sum(second * d_mix, axis=-1, keepdims=True)))).astype(jnp.bfloat16)
    q_first = (jnp.dot(d_first, key_rows[:, 0], preferred_element_type=jnp.float32) * factor).astype(jnp.bfloat16)
    q_second = (jnp.dot(d_second, key_rows[:, 1], preferred_element_type=jnp.float32) * factor).astype(jnp.bfloat16)
    return (jnp.stack([q_first, q_second], axis=1).reshape(length, 2 * head_dim), d_value)

def reference(inputs, queries, keys, values, head_cot, mixing, head_gain, factors, moments, weights):
    sequences = TOKENS // TOK_DEV
    query_all = queries.reshape(sequences, TOK_DEV, HEADS, 2, HEAD_DIM)
    key_all = keys.reshape(sequences, TOK_DEV, HEADS, 2, HEAD_DIM)
    value_all = values.reshape(sequences, TOK_DEV, HEADS, 2 * HEAD_DIM)
    upstream_all = head_cot.reshape(sequences, TOK_DEV, HEADS, 2 * HEAD_DIM)
    per_head = jax.vmap(head_grads, in_axes=(1, 1, 1, 1, 0, None))

    def one_sequence(pieces):
        return per_head(pieces[0], pieces[1], pieces[2], pieces[3], mixing, head_gain)
    d_query, d_value = lax.map(one_sequence, (query_all, key_all, value_all, upstream_all))
    d_query = d_query.transpose(0, 2, 1, 3).reshape(TOKENS, HV)
    d_value = d_value.transpose(0, 2, 1, 3).reshape(TOKENS, HV)
    cotangents = jnp.stack([d_query, d_value], axis=1).reshape(TOKENS, 2 * HV)
    grads = jnp.dot(inputs.T, cotangents, preferred_element_type=jnp.float32).reshape(D, 2, HV)
    grads = grads * TOKENS ** (-0.5)
    factor_wide = factors.astype(jnp.float32)
    projected = jnp.einsum('dkr,dke->rke', factor_wide, grads, precision=lax.Precision.HIGHEST)
    new_moments = BETA * moments + projected
    totals = lax.optimization_barrier(jnp.sum(new_moments * new_moments, axis=(0, 2)))
    rate = RATE_BASE / jnp.sqrt(1.0 + totals / (RANK * HV))
    step = jnp.einsum('dkr,rke->dke', factor_wide, new_moments, precision=lax.Precision.HIGHEST) * rate[None, :, None]
    copies = (weights - step).astype(jnp.bfloat16)
    return (step, new_moments, copies)
```

```python
import functools

import jax
import jax.numpy as jnp
from jax import lax
from jax.experimental import pallas as pl
from jax.experimental.pallas import tpu as pltpu
from jax.sharding import PartitionSpec as P

EPS = 0.05
BETA = 0.9
RATE_BASE = 0.5
MESH = pl.DeviceIdType.MESH


class Gather:
    def __init__(self, n, own, slot, send, recv):
        me = lax.axis_index("fs")
        self.own, self.slot, self.send, self.recv = own, slot, send, recv
        self.n, self.me, self.places = n, me, n // 2
        self.place, self.parity = me // 2, me % 2
        self.partner = me + 1 - 2 * self.parity
        self.started = []

    def put(self, cond, index, half, way):
        target = (self.me - 2, self.me + 2, self.partner)[way]
        if way == 0:
            cond = jnp.logical_and(cond, self.place > 0)
        elif way == 1:
            cond = jnp.logical_and(cond, self.place < self.places - 1)
        mine = index is self.me

        def make():
            return pltpu.make_async_remote_copy(
                src_ref=self.own(half) if mine else self.slot(index, half),
                dst_ref=self.slot(index, half),
                send_sem=self.send.at[index, half, way],
                recv_sem=self.recv.at[index, half],
                device_id={"fs": target},
                device_id_type=MESH,
            )

        @pl.when(cond)
        def _():
            make().start()

        self.started.append((cond, make))

    def arrive(self, cond, index, half):
        @pl.when(cond)
        def _():
            pltpu.make_async_remote_copy(
                src_ref=self.slot(index, half),
                dst_ref=self.slot(index, half),
                send_sem=self.send.at[index, half, 0],
                recv_sem=self.recv.at[index, half],
                device_id={"fs": self.partner},
                device_id_type=MESH,
            ).wait_recv()

    def begin(self):
        true = self.me >= 0
        for half in (0, 1):
            for way in (2, 0, 1):
                self.put(true, self.me, half, way)

    def turn(self):
        true = self.me >= 0
        self.arrive(true, self.partner, 0)
        for way in (0, 1):
            self.put(true, self.partner, 0, way)

    def step(self, s):
        for way in (1, 0):
            place = self.place - s if way == 1 else self.place + s
            cond = jnp.logical_and(place >= 0, place < self.places)
            same = 2 * place + self.parity
            other = 2 * place + 1 - self.parity
            self.arrive(cond, same, 1)
            self.put(cond, same, 1, 2)
            self.put(cond, same, 1, way)
            self.arrive(cond, same, 0)
            self.put(cond, same, 0, way)
            self.arrive(cond, other, 0)
            self.put(cond, other, 0, way)

    def finish_recv(self):
        true = self.me >= 0
        for place in range(self.places):
            self.arrive(true, 2 * place + 1 - self.parity, 1)

    def finish_send(self):
        for cond, make in self.started:

            @pl.when(cond)
            def _(make=make):
                make().wait_send()


def head_step(head, q_ref, k_ref, v_ref, c_ref, mix_ref, gain_ref, dq_ref, dv_ref):
    length = q_ref.shape[0]
    width = gain_ref.shape[1]
    half = width // 2
    factor = half ** (-0.5)
    cols = slice(head * width, (head + 1) * width)
    query, key, value = q_ref[:, cols], k_ref[:, cols], v_ref[:, cols]
    lane = lax.broadcasted_iota(jnp.int32, (length, width), 1)
    zero = jnp.zeros_like(key)
    key0 = jnp.where(lane < half, key, zero)
    key1 = jnp.where(lane < half, zero, key)
    row = lax.broadcasted_iota(jnp.int32, (length, length), 0)
    col = lax.broadcasted_iota(jnp.int32, (length, length), 1)
    causal = col <= row
    mix = mix_ref[head]
    nt = (((1,), (1,)), ((), ()))
    tn = (((0,), (0,)), ((), ()))

    def probs(rows):
        scores = lax.dot_general(query, rows, nt, preferred_element_type=jnp.float32) * factor
        scores = jnp.where(causal, scores, -jnp.inf)
        expo = jnp.exp(scores - jnp.max(scores, axis=-1, keepdims=True))
        return expo * (1.0 / jnp.sum(expo, axis=-1, keepdims=True))

    first, second = probs(key0), probs(key1)
    mixed = (first - mix * second).astype(jnp.bfloat16)
    output = jnp.dot(mixed, value, preferred_element_type=jnp.float32)
    inverse = lax.rsqrt(jnp.mean(output * output, axis=-1, keepdims=True) + EPS)
    scaled = gain_ref[...] * c_ref[:, cols].astype(jnp.float32)
    d_out = inverse * scaled - output * (inverse * inverse * inverse) * jnp.mean(
        output * scaled, axis=-1, keepdims=True
    )
    d_out = d_out.astype(jnp.bfloat16)
    dv_ref[:, cols] = lax.dot_general(mixed, d_out, tn, preferred_element_type=jnp.float32).astype(jnp.bfloat16)
    d_mix = lax.dot_general(d_out, value, nt, preferred_element_type=jnp.float32)
    d_first = first * (d_mix - jnp.sum(first * d_mix, axis=-1, keepdims=True))
    d_second = -mix * second * (d_mix - jnp.sum(second * d_mix, axis=-1, keepdims=True))
    d_query = jnp.dot(d_first.astype(jnp.bfloat16), key0, preferred_element_type=jnp.float32)
    d_query += jnp.dot(d_second.astype(jnp.bfloat16), key1, preferred_element_type=jnp.float32)
    dq_ref[:, cols] = (d_query * factor).astype(jnp.bfloat16)


def kernel(
    n, tp, heads,
    x_ref, q_ref, k_ref, v_ref, c_ref, mix_ref, gain_ref, f_ref, mom_ref, w_ref,
    fall, wall, nmall, nm_ref, tot_ref,
    dq, dv, psend, precv, sums,
    f_send, f_recv, w_send, w_recv, n_send, n_recv, p_send, p_recv, t_send, t_recv,
):
    me = lax.axis_index("fs")
    mt = lax.axis_index("tp")
    barrier = pltpu.get_barrier_semaphore()
    for hop in range(1, n):
        pl.semaphore_signal(barrier, inc=1, device_id={"fs": (me + hop) % n}, device_id_type=MESH)
    for hop in range(1, tp):
        pl.semaphore_signal(barrier, inc=1, device_id={"tp": (mt + hop) % tp}, device_id_type=MESH)
    pl.semaphore_wait(barrier, n - 1 + tp - 1)

    deep = f_ref.shape[0]
    part = deep // 2
    rank = f_ref.shape[1] // 2
    rank_here = rank // n

    def rows(ref):
        def slot(index, half):
            return ref.at[pl.ds(pl.multiple_of(index * deep + half * part, part), part)]

        return slot

    def own(ref):
        return lambda half: ref.at[pl.ds(half * part, part)]

    gather_f = Gather(n, own(f_ref), rows(fall), f_send, f_recv)
    gather_w = Gather(n, own(w_ref), rows(wall), w_send, w_recv)
    gather_n = Gather(
        n, lambda half: nmall.at[me, half], lambda i, half: nmall.at[i, half], n_send, n_recv
    )
    gather_f.begin()
    gather_w.begin()
    here = pl.ds(pl.multiple_of(me * deep, deep), deep)
    fall[here, :] = f_ref[...]
    wall[here, :] = w_ref[...]
    gather_f.turn()
    done = 1
    for head in range(heads):
        head_step(head, q_ref, k_ref, v_ref, c_ref, mix_ref, gain_ref, dq, dv)
        if done < n // 2:
            gather_f.step(done)
            done += 1
    for s in range(done, n // 2):
        gather_f.step(s)
    gather_w.turn()
    gather_f.finish_recv()
    gather_w.step(1)
    for m, cot in enumerate((dq, dv)):
        reduced = jnp.dot(
            x_ref[...], fall[:, m * rank : (m + 1) * rank], preferred_element_type=jnp.float32
        ).astype(jnp.bfloat16)
        partial = lax.dot_general(
            reduced, cot[...], (((0,), (0,)), ((), ())), preferred_element_type=jnp.float32
        )
        for j in range(n):
            psend[j, m] = partial[j * rank_here : (j + 1) * rank_here].astype(psend.dtype)

    def p_copy(hop):
        peer = (me + hop) % n
        return pltpu.make_async_remote_copy(
            src_ref=psend.at[peer],
            dst_ref=precv.at[hop],
            send_sem=p_send.at[hop],
            recv_sem=p_recv.at[hop],
            device_id={"fs": peer},
            device_id_type=MESH,
        )

    for hop in range(1, n):
        p_copy(hop).start()
    for s in range(2, n // 2 - 1):
        gather_w.step(s)
    total = psend[me].astype(jnp.float32)
    for hop in range(1, n):
        p_copy(hop).wait_recv()
        total += precv[hop].astype(jnp.float32)
    length = x_ref.shape[0]
    moments = BETA * mom_ref[...] + total * (length * n) ** (-0.5)
    nm_ref[...] = moments
    nmall[me] = moments.astype(nmall.dtype)
    gather_n.begin()
    gather_w.step(n // 2 - 1)
    gather_n.turn()
    for s in range(1, n // 2):
        gather_n.step(s)
    gather_n.finish_recv()
    everything = nmall[...].astype(jnp.float32)
    squares = jnp.sum(jnp.sum(everything * everything, axis=0), axis=1)
    sums[0] = jnp.sum(squares, axis=1, keepdims=True) + jnp.zeros((2, 128), jnp.float32)

    def t_copy(hop):
        return pltpu.make_async_remote_copy(
            src_ref=sums.at[0],
            dst_ref=sums.at[hop],
            send_sem=t_send.at[hop],
            recv_sem=t_recv.at[hop],
            device_id={"tp": (mt + hop) % tp},
            device_id_type=MESH,
        )

    for hop in range(1, tp):
        t_copy(hop).start()
    gather_w.finish_recv()
    totals = sums[0]
    for hop in range(1, tp):
        t_copy(hop).wait_recv()
        totals += sums[hop]
    tot_ref[...] = totals
    for hop in range(1, tp):
        t_copy(hop).wait_send()
    for hop in range(1, n):
        p_copy(hop).wait_send()
    for gather in (gather_f, gather_w, gather_n):
        gather.finish_send()


def per_device(
    n, tp, inputs, queries, keys, values, head_cot, mixing, head_gain, factors, moments, weights
):
    length, depth = inputs.shape
    heads = mixing.shape[0]
    deep, _, rank = factors.shape
    rank_here, _, cols = moments.shape
    wire = jnp.bfloat16 if rank_here % 16 == 0 else jnp.float32
    vmem = pl.BlockSpec(memory_space=pltpu.VMEM)
    dma = pltpu.SemaphoreType.DMA
    f_flat = factors.reshape(deep, 2 * rank)
    w_flat = weights.astype(jnp.bfloat16).reshape(deep, 2 * cols)
    mom = moments.transpose(1, 0, 2)
    fall, wall, nmall, nm, totals = pl.pallas_call(
        functools.partial(kernel, n, tp, heads),
        out_shape=(
            jax.ShapeDtypeStruct((depth, 2 * rank), jnp.bfloat16),
            jax.ShapeDtypeStruct((depth, 2 * cols), jnp.bfloat16),
            jax.ShapeDtypeStruct((n, 2, rank_here, cols), wire),
            jax.ShapeDtypeStruct((2, rank_here, cols), jnp.float32),
            jax.ShapeDtypeStruct((2, 128), jnp.float32),
        ),
        in_specs=[vmem] * 5 + [pl.BlockSpec(memory_space=pltpu.SMEM)] + [vmem] * 4,
        out_specs=(vmem,) * 5,
        scratch_shapes=[
            pltpu.VMEM((length, cols), jnp.bfloat16),
            pltpu.VMEM((length, cols), jnp.bfloat16),
            pltpu.VMEM((n, 2, rank_here, cols), wire),
            pltpu.VMEM((n, 2, rank_here, cols), wire),
            pltpu.VMEM((tp, 2, 128), jnp.float32),
            dma((n, 2, 3)), dma((n, 2)),
            dma((n, 2, 3)), dma((n, 2)),
            dma((n, 2, 3)), dma((n, 2)),
            dma((n,)), dma((n,)),
            dma((tp,)), dma((tp,)),
        ],
        compiler_params=pltpu.CompilerParams(
            collective_id=0, has_side_effects=True, vmem_limit_bytes=56 * 1024 * 1024
        ),
    )(inputs, queries, keys, values, head_cot, mixing, head_gain[None, :], f_flat, mom, w_flat)
    rate = RATE_BASE / jnp.sqrt(1.0 + totals[:, 0] / (rank * cols * tp))
    steps, copies = [], []
    for m in range(2):
        block = nmall[:, m].reshape(rank, cols).astype(jnp.bfloat16)
        steps.append(
            jnp.dot(factors[:, m], block, preferred_element_type=jnp.float32) * rate[m]
        )
        low = jnp.dot(
            fall[:, m * rank : (m + 1) * rank], block, preferred_element_type=jnp.float32
        )
        copies.append(
            (wall[:, m * cols : (m + 1) * cols].astype(jnp.float32) - low * rate[m]).astype(
                jnp.bfloat16
            )
        )
    return jnp.stack(steps, axis=1), nm.transpose(1, 0, 2), jnp.stack(copies, axis=1)


def solution(mesh):
    placed = (
        P("fs", None),
        P("fs", "tp"),
        P("fs", "tp"),
        P("fs", "tp"),
        P("fs", "tp"),
        P("tp"),
        P(),
        P("fs", None, None),
        P("fs", None, "tp"),
        P("fs", None, "tp"),
    )
    return jax.shard_map(
        functools.partial(per_device, mesh.shape["fs"], mesh.shape["tp"]),
        mesh=mesh,
        in_specs=placed,
        out_specs=(P("fs", None, "tp"), P("fs", None, "tp"), P(None, None, "tp")),
        check_vma=False,
    )
```

```python
import functools

import jax
import jax.numpy as jnp
from jax import lax
from jax.experimental import pallas as pl
from jax.experimental.pallas import tpu as pltpu
from jax.sharding import PartitionSpec as P

EPS = 0.05
BETA = 0.9
RATE_BASE = 0.5
MESH = pl.DeviceIdType.MESH
LANES = 128


class Gather:
    def __init__(self, n, slot, send, recv):
        me = lax.axis_index("fs")
        self.slot, self.send, self.recv = slot, send, recv
        self.n, self.me, self.places = n, me, n // 2
        self.place, self.parity = me // 2, me % 2
        self.partner = me + 1 - 2 * self.parity
        self.started = []

    def put(self, cond, index, half, way):
        target = (self.me - 2, self.me + 2, self.partner)[way]
        if way == 0:
            cond = jnp.logical_and(cond, self.place > 0)
        elif way == 1:
            cond = jnp.logical_and(cond, self.place < self.places - 1)

        def make():
            return pltpu.make_async_remote_copy(
                src_ref=self.slot(index, half),
                dst_ref=self.slot(index, half),
                send_sem=self.send.at[index, half, way],
                recv_sem=self.recv.at[index, half],
                device_id={"fs": target},
                device_id_type=MESH,
            )

        @pl.when(cond)
        def _():
            make().start()

        self.started.append((cond, make))

    def arrive(self, cond, index, half):
        @pl.when(cond)
        def _():
            pltpu.make_async_remote_copy(
                src_ref=self.slot(index, half),
                dst_ref=self.slot(index, half),
                send_sem=self.send.at[index, half, 0],
                recv_sem=self.recv.at[index, half],
                device_id={"fs": self.partner},
                device_id_type=MESH,
            ).wait_recv()

    def begin(self):
        true = self.me >= 0
        for half in (0, 1):
            for way in (2, 0, 1):
                self.put(true, self.me, half, way)

    def turn(self):
        true = self.me >= 0
        self.arrive(true, self.partner, 0)
        for way in (0, 1):
            self.put(true, self.partner, 0, way)

    def step(self, s):
        for way in (1, 0):
            place = self.place - s if way == 1 else self.place + s
            cond = jnp.logical_and(place >= 0, place < self.places)
            same = 2 * place + self.parity
            other = 2 * place + 1 - self.parity
            self.arrive(cond, same, 1)
            self.put(cond, same, 1, 2)
            self.put(cond, same, 1, way)
            self.arrive(cond, same, 0)
            self.put(cond, same, 0, way)
            self.arrive(cond, other, 0)
            self.put(cond, other, 0, way)

    def finish_recv(self):
        true = self.me >= 0
        for place in range(self.places):
            self.arrive(true, 2 * place + 1 - self.parity, 1)

    def finish_send(self):
        for cond, make in self.started:

            @pl.when(cond)
            def _(make=make):
                make().wait_send()


def split(ref, t, tiles, count):
    return ref[pl.ds(t % tiles * 2 + t // tiles, count, stride=2 * tiles), :]


def head_step(head, q_ref, k_ref, v_ref, c_ref, mix_ref, gain_ref, dq_ref, dv_ref):
    length = q_ref.shape[0]
    width = gain_ref.shape[1]
    half = width // 2
    factor = half ** (-0.5)
    cols = slice(head * width, (head + 1) * width)
    query, key, value = q_ref[:, cols], k_ref[:, cols], v_ref[:, cols]
    lane = lax.broadcasted_iota(jnp.int32, (length, width), 1)
    zero = jnp.zeros_like(key)
    key0 = jnp.where(lane < half, key, zero)
    key1 = jnp.where(lane < half, zero, key)
    row = lax.broadcasted_iota(jnp.int32, (length, length), 0)
    col = lax.broadcasted_iota(jnp.int32, (length, length), 1)
    causal = col <= row
    mix = mix_ref[head]
    nt = (((1,), (1,)), ((), ()))
    tn = (((0,), (0,)), ((), ()))

    def probs(rows):
        scores = lax.dot_general(query, rows, nt, preferred_element_type=jnp.float32) * factor
        scores = jnp.where(causal, scores, -jnp.inf)
        expo = jnp.exp(scores - jnp.max(scores, axis=-1, keepdims=True))
        return expo * (1.0 / jnp.sum(expo, axis=-1, keepdims=True))

    first, second = probs(key0), probs(key1)
    mixed = (first - mix * second).astype(jnp.bfloat16)
    output = jnp.dot(mixed, value, preferred_element_type=jnp.float32)
    inverse = lax.rsqrt(jnp.mean(output * output, axis=-1, keepdims=True) + EPS)
    scaled = gain_ref[...] * c_ref[:, cols].astype(jnp.float32)
    d_out = inverse * scaled - output * (inverse * inverse * inverse) * jnp.mean(
        output * scaled, axis=-1, keepdims=True
    )
    d_out = d_out.astype(jnp.bfloat16)
    dv_ref[:, cols] = lax.dot_general(mixed, d_out, tn, preferred_element_type=jnp.float32).astype(jnp.bfloat16)
    d_mix = lax.dot_general(d_out, value, nt, preferred_element_type=jnp.float32)
    d_first = first * (d_mix - jnp.sum(first * d_mix, axis=-1, keepdims=True))
    d_second = -mix * second * (d_mix - jnp.sum(second * d_mix, axis=-1, keepdims=True))
    d_query = jnp.dot(d_first.astype(jnp.bfloat16), key0, preferred_element_type=jnp.float32)
    d_query += jnp.dot(d_second.astype(jnp.bfloat16), key1, preferred_element_type=jnp.float32)
    dq_ref[:, cols] = (d_query * factor).astype(jnp.bfloat16)


def kernel(
    n, tp, heads,
    x_ref, q_ref, k_ref, v_ref, c_ref, mix_ref, gain_ref, f_ref, mom_ref, w_ref,
    fall, wall, nmall, nm_ref, tot_ref, fown,
    fwide, dq, dv, psend, precv, sums,
    f_send, f_recv, w_send, w_recv, n_send, n_recv, p_send, p_recv, t_send, t_recv,
):
    me = lax.axis_index("fs")
    mt = lax.axis_index("tp")
    deep = fown.shape[0]
    part = deep // 2
    rank = fown.shape[1] // 2
    rank_here = rank // n
    cols = dq.shape[1]
    tiles_f, tiles_w = rank // LANES, cols // LANES
    here = pl.ds(pl.multiple_of(me * deep, deep), deep)
    fwide[...] = f_ref[...].astype(jnp.float32)
    for t in range(2 * tiles_f):
        block = split(fwide, t, tiles_f, deep).astype(jnp.bfloat16)
        fown[:, t * LANES : (t + 1) * LANES] = block
        fall[here, t * LANES : (t + 1) * LANES] = block
    barrier = pltpu.get_barrier_semaphore()
    for hop in range(1, n):
        pl.semaphore_signal(barrier, inc=1, device_id={"fs": (me + hop) % n}, device_id_type=MESH)
    for hop in range(1, tp):
        pl.semaphore_signal(barrier, inc=1, device_id={"tp": (mt + hop) % tp}, device_id_type=MESH)
    pl.semaphore_wait(barrier, n - 1 + tp - 1)

    def rows(ref):
        def slot(index, half):
            return ref.at[pl.ds(pl.multiple_of(index * deep + half * part, part), part)]

        return slot

    gather_f = Gather(n, rows(fall), f_send, f_recv)
    gather_w = Gather(n, rows(wall), w_send, w_recv)
    gather_n = Gather(n, lambda i, half: nmall.at[i, half], n_send, n_recv)
    gather_f.begin()
    for t in range(2 * tiles_w):
        wall[here, t * LANES : (t + 1) * LANES] = split(w_ref, t, tiles_w, deep).astype(jnp.bfloat16)
    gather_w.begin()
    gather_f.turn()
    done = 1
    for head in range(heads):
        head_step(head, q_ref, k_ref, v_ref, c_ref, mix_ref, gain_ref, dq, dv)
        if done < n // 2:
            gather_f.step(done)
            done += 1
    for s in range(done, n // 2):
        gather_f.step(s)
    gather_w.turn()
    gather_f.finish_recv()
    gather_w.step(1)
    for m, cot in enumerate((dq, dv)):
        reduced = jnp.dot(
            x_ref[...], fall[:, m * rank : (m + 1) * rank], preferred_element_type=jnp.float32
        ).astype(jnp.bfloat16)
        partial = lax.dot_general(
            reduced, cot[...], (((0,), (0,)), ((), ())), preferred_element_type=jnp.float32
        )
        for j in range(n):
            psend[j, m] = partial[j * rank_here : (j + 1) * rank_here].astype(psend.dtype)

    def p_copy(hop):
        peer = (me + hop) % n
        return pltpu.make_async_remote_copy(
            src_ref=psend.at[peer],
            dst_ref=precv.at[hop],
            send_sem=p_send.at[hop],
            recv_sem=p_recv.at[hop],
            device_id={"fs": peer},
            device_id_type=MESH,
        )

    for hop in range(1, n):
        p_copy(hop).start()
    for s in range(2, n // 2 - 1):
        gather_w.step(s)
    total = psend[me].astype(jnp.float32)
    for hop in range(1, n):
        p_copy(hop).wait_recv()
        total += precv[hop].astype(jnp.float32)
    length = x_ref.shape[0]
    for t in range(2 * tiles_w):
        m, lanes = t // tiles_w, slice(t % tiles_w * LANES, (t % tiles_w + 1) * LANES)
        moments = BETA * split(mom_ref, t, tiles_w, rank_here)
        moments += total[m, :, lanes] * (length * n) ** (-0.5)
        nm_ref[m, :, lanes] = moments
        nmall[me, m, :, lanes] = moments.astype(nmall.dtype)
    gather_n.begin()
    gather_w.step(n // 2 - 1)
    gather_n.turn()
    for s in range(1, n // 2):
        gather_n.step(s)
    gather_n.finish_recv()
    everything = nmall[...].astype(jnp.float32)
    squares = jnp.sum(jnp.sum(everything * everything, axis=0), axis=1)
    sums[0] = jnp.sum(squares, axis=1, keepdims=True) + jnp.zeros((2, 128), jnp.float32)

    def t_copy(hop):
        return pltpu.make_async_remote_copy(
            src_ref=sums.at[0],
            dst_ref=sums.at[hop],
            send_sem=t_send.at[hop],
            recv_sem=t_recv.at[hop],
            device_id={"tp": (mt + hop) % tp},
            device_id_type=MESH,
        )

    for hop in range(1, tp):
        t_copy(hop).start()
    gather_w.finish_recv()
    totals = sums[0]
    for hop in range(1, tp):
        t_copy(hop).wait_recv()
        totals += sums[hop]
    tot_ref[...] = totals
    for hop in range(1, tp):
        t_copy(hop).wait_send()
    for hop in range(1, n):
        p_copy(hop).wait_send()
    for gather in (gather_f, gather_w, gather_n):
        gather.finish_send()


def finish(entries, fall, wall, nmall, nm_ref, tot_ref, fown, step, nm_out, copies, wide):
    _, _, rank_here, cols = nmall.shape
    rank = fall.shape[1] // 2
    tiles = cols // LANES
    rate = RATE_BASE / jnp.sqrt(1.0 + tot_ref[...] / entries)

    def lows(rows, m):
        block = nmall[:, m].reshape(rank, cols).astype(jnp.bfloat16)
        return jnp.dot(
            rows[:, m * rank : (m + 1) * rank], block, preferred_element_type=jnp.float32
        )

    count = fall.shape[0]
    for m in range(2):
        low = lows(fall, m)
        for t in range(tiles):
            lanes = slice(t * LANES, (t + 1) * LANES)
            old = wall[:, m * cols + t * LANES : m * cols + (t + 1) * LANES].astype(jnp.float32)
            wide[pl.ds(2 * t + m, count, stride=2 * tiles), :] = (
                old - low[:, lanes] * rate[m : m + 1]
            )
    copies[...] = wide[...].astype(jnp.bfloat16)

    @pl.when(pl.program_id(0) == 0)
    def _():
        for m in range(2):
            low = lows(fown, m)
            for t in range(tiles):
                lanes = slice(t * LANES, (t + 1) * LANES)
                step[pl.ds(2 * t + m, fown.shape[0], stride=2 * tiles), :] = (
                    low[:, lanes] * rate[m : m + 1]
                )
                nm_out[pl.ds(2 * t + m, rank_here, stride=2 * tiles), :] = nm_ref[m, :, lanes]


def to_rows(array):
    rows, maps, cols = array.shape
    return array.reshape(rows, maps, cols // LANES, LANES).transpose(0, 2, 1, 3).reshape(-1, LANES)


def from_rows(array, rows):
    return (
        array.reshape(rows, -1, 2, LANES).transpose(0, 2, 1, 3).reshape(rows, 2, -1)
    )


def per_device(
    n, tp, inputs, queries, keys, values, head_cot, mixing, head_gain, factors, moments, weights
):
    length, depth = inputs.shape
    heads = mixing.shape[0]
    deep, _, rank = factors.shape
    rank_here, _, cols = moments.shape
    wire = jnp.bfloat16 if rank_here % 16 == 0 else jnp.float32
    vmem = pl.BlockSpec(memory_space=pltpu.VMEM)
    dma = pltpu.SemaphoreType.DMA
    held = pl.pallas_call(
        functools.partial(kernel, n, tp, heads),
        out_shape=(
            jax.ShapeDtypeStruct((depth, 2 * rank), jnp.bfloat16),
            jax.ShapeDtypeStruct((depth, 2 * cols), jnp.bfloat16),
            jax.ShapeDtypeStruct((n, 2, rank_here, cols), wire),
            jax.ShapeDtypeStruct((2, rank_here, cols), jnp.float32),
            jax.ShapeDtypeStruct((2, LANES), jnp.float32),
            jax.ShapeDtypeStruct((deep, 2 * rank), jnp.bfloat16),
        ),
        in_specs=[vmem] * 5 + [pl.BlockSpec(memory_space=pltpu.SMEM)] + [vmem] * 4,
        out_specs=(vmem,) * 6,
        scratch_shapes=[
            pltpu.VMEM((deep * 2 * rank // LANES, LANES), jnp.float32),
            pltpu.VMEM((length, cols), jnp.bfloat16),
            pltpu.VMEM((length, cols), jnp.bfloat16),
            pltpu.VMEM((n, 2, rank_here, cols), wire),
            pltpu.VMEM((n, 2, rank_here, cols), wire),
            pltpu.VMEM((tp, 2, LANES), jnp.float32),
            dma((n, 2, 3)), dma((n, 2)),
            dma((n, 2, 3)), dma((n, 2)),
            dma((n, 2, 3)), dma((n, 2)),
            dma((n,)), dma((n,)),
            dma((tp,)), dma((tp,)),
        ],
        compiler_params=pltpu.CompilerParams(
            collective_id=0, has_side_effects=True, vmem_limit_bytes=56 * 1024 * 1024
        ),
    )(
        inputs, queries, keys, values, head_cot, mixing, head_gain[None, :],
        to_rows(factors), to_rows(moments), to_rows(weights),
    )
    block = min(depth, 256)
    per_row = 2 * cols // LANES

    def whole(shape):
        return pl.BlockSpec(shape, lambda i: (0,) * len(shape))

    step, new_moments, copies = pl.pallas_call(
        functools.partial(finish, rank * cols * tp),
        grid=(depth // block,),
        out_shape=(
            jax.ShapeDtypeStruct((deep * per_row, LANES), jnp.float32),
            jax.ShapeDtypeStruct((rank_here * per_row, LANES), jnp.float32),
            jax.ShapeDtypeStruct((depth * per_row, LANES), jnp.bfloat16),
        ),
        in_specs=[
            pl.BlockSpec((block, 2 * rank), lambda i: (i, 0)),
            pl.BlockSpec((block, 2 * cols), lambda i: (i, 0)),
            whole((n, 2, rank_here, cols)),
            whole((2, rank_here, cols)),
            whole((2, LANES)),
            whole((deep, 2 * rank)),
        ],
        out_specs=(
            whole((deep * per_row, LANES)),
            whole((rank_here * per_row, LANES)),
            pl.BlockSpec((block * per_row, LANES), lambda i: (i, 0)),
        ),
        scratch_shapes=[pltpu.VMEM((block * per_row, LANES), jnp.float32)],
    )(*held)
    return from_rows(step, deep), from_rows(new_moments, rank_here), from_rows(copies, depth)


def solution(mesh):
    placed = (
        P("fs", None),
        P("fs", "tp"),
        P("fs", "tp"),
        P("fs", "tp"),
        P("fs", "tp"),
        P("tp"),
        P(),
        P("fs", None, None),
        P("fs", None, "tp"),
        P("fs", None, "tp"),
    )
    return jax.shard_map(
        functools.partial(per_device, mesh.shape["fs"], mesh.shape["tp"]),
        mesh=mesh,
        in_specs=placed,
        out_specs=(P("fs", None, "tp"), P("fs", None, "tp"), P(None, None, "tp")),
        check_vma=False,
    )
```

```python
import functools

import jax
import jax.numpy as jnp
from jax import lax
from jax.experimental import pallas as pl
from jax.experimental.pallas import tpu as pltpu
from jax.sharding import PartitionSpec as P

EPS = 0.05
BETA = 0.9
RATE_BASE = 0.5
MESH = pl.DeviceIdType.MESH
LANES = 128


class Gather:
    def __init__(self, n, slot, send, recv, hook=None):
        me = lax.axis_index("fs")
        self.slot, self.send, self.recv, self.hook = slot, send, recv, hook
        self.n, self.me, self.places = n, me, n // 2
        self.place, self.parity = me // 2, me % 2
        self.partner = me + 1 - 2 * self.parity
        self.started = []

    def put(self, cond, index, half, way):
        target = (self.me - 2, self.me + 2, self.partner)[way]
        if way == 0:
            cond = jnp.logical_and(cond, self.place > 0)
        elif way == 1:
            cond = jnp.logical_and(cond, self.place < self.places - 1)

        def make():
            return pltpu.make_async_remote_copy(
                src_ref=self.slot(index, half),
                dst_ref=self.slot(index, half),
                send_sem=self.send.at[index, half, way],
                recv_sem=self.recv.at[index, half],
                device_id={"fs": target},
                device_id_type=MESH,
            )

        @pl.when(cond)
        def _():
            make().start()

        self.started.append((cond, make))

    def arrive(self, cond, index, half):
        @pl.when(cond)
        def _():
            pltpu.make_async_remote_copy(
                src_ref=self.slot(index, half),
                dst_ref=self.slot(index, half),
                send_sem=self.send.at[index, half, 0],
                recv_sem=self.recv.at[index, half],
                device_id={"fs": self.partner},
                device_id_type=MESH,
            ).wait_recv()
            if self.hook is not None:
                self.hook(index, half)

    def begin(self):
        true = self.me >= 0
        for half in (0, 1):
            for way in (2, 0, 1):
                self.put(true, self.me, half, way)

    def turn(self):
        true = self.me >= 0
        self.arrive(true, self.partner, 0)
        for way in (0, 1):
            self.put(true, self.partner, 0, way)

    def step(self, s):
        for way in (1, 0):
            place = self.place - s if way == 1 else self.place + s
            cond = jnp.logical_and(place >= 0, place < self.places)
            same = 2 * place + self.parity
            other = 2 * place + 1 - self.parity
            self.arrive(cond, same, 1)
            self.put(cond, same, 1, 2)
            self.put(cond, same, 1, way)
            self.arrive(cond, same, 0)
            self.put(cond, same, 0, way)
            self.arrive(cond, other, 0)
            self.put(cond, other, 0, way)

    def finish_recv(self):
        true = self.me >= 0
        for place in range(self.places):
            self.arrive(true, 2 * place + 1 - self.parity, 1)

    def finish_send(self):
        for cond, make in self.started:

            @pl.when(cond)
            def _(make=make):
                make().wait_send()


def split(ref, t, tiles, count):
    return ref[pl.ds(t % tiles * 2 + t // tiles, count, stride=2 * tiles), :]


def head_step(head, q_ref, k_ref, v_ref, c_ref, mix_ref, gain_ref, dq_ref, dv_ref):
    length = q_ref.shape[0]
    width = gain_ref.shape[1]
    half = width // 2
    factor = half ** (-0.5)
    cols = slice(head * width, (head + 1) * width)
    query, key, value = q_ref[:, cols], k_ref[:, cols], v_ref[:, cols]
    lane = lax.broadcasted_iota(jnp.int32, (length, width), 1)
    zero = jnp.zeros_like(key)
    key0 = jnp.where(lane < half, key, zero)
    key1 = jnp.where(lane < half, zero, key)
    row = lax.broadcasted_iota(jnp.int32, (length, length), 0)
    col = lax.broadcasted_iota(jnp.int32, (length, length), 1)
    causal = col <= row
    mix = mix_ref[head]
    nt = (((1,), (1,)), ((), ()))
    tn = (((0,), (0,)), ((), ()))

    def probs(rows):
        scores = lax.dot_general(query, rows, nt, preferred_element_type=jnp.float32) * factor
        scores = jnp.where(causal, scores, -jnp.inf)
        expo = jnp.exp(scores - jnp.max(scores, axis=-1, keepdims=True))
        return expo * (1.0 / jnp.sum(expo, axis=-1, keepdims=True))

    first, second = probs(key0), probs(key1)
    mixed = (first - mix * second).astype(jnp.bfloat16)
    output = jnp.dot(mixed, value, preferred_element_type=jnp.float32)
    inverse = lax.rsqrt(jnp.mean(output * output, axis=-1, keepdims=True) + EPS)
    scaled = gain_ref[...] * c_ref[:, cols].astype(jnp.float32)
    d_out = inverse * scaled - output * (inverse * inverse * inverse) * jnp.mean(
        output * scaled, axis=-1, keepdims=True
    )
    d_out = d_out.astype(jnp.bfloat16)
    dv_ref[:, cols] = lax.dot_general(mixed, d_out, tn, preferred_element_type=jnp.float32).astype(jnp.bfloat16)
    d_mix = lax.dot_general(d_out, value, nt, preferred_element_type=jnp.float32)
    d_first = first * (d_mix - jnp.sum(first * d_mix, axis=-1, keepdims=True))
    d_second = -mix * second * (d_mix - jnp.sum(second * d_mix, axis=-1, keepdims=True))
    d_query = jnp.dot(d_first.astype(jnp.bfloat16), key0, preferred_element_type=jnp.float32)
    d_query += jnp.dot(d_second.astype(jnp.bfloat16), key1, preferred_element_type=jnp.float32)
    dq_ref[:, cols] = (d_query * factor).astype(jnp.bfloat16)


def kernel(
    n, tp, heads,
    x_ref, q_ref, k_ref, v_ref, c_ref, mix_ref, gain_ref, f_ref, mom_ref, w_ref,
    fall, wall, nmall, nm_ref, tot_ref, fown,
    fwide, dq, dv, psend, precv, sums,
    f_send, f_recv, s_send, s_recv, w_send, w_recv, n_send, n_recv, p_send, p_recv, t_send, t_recv,
):
    me = lax.axis_index("fs")
    mt = lax.axis_index("tp")
    deep = fown.shape[0]
    part = deep // 2
    rank = fown.shape[1] // 2
    rank_here = rank // n
    cols = dq.shape[1]
    tiles_f, tiles_w = rank // LANES, cols // LANES
    here = pl.ds(pl.multiple_of(me * deep, deep), deep)
    fwide[...] = f_ref[...].astype(jnp.float32)
    for t in range(2 * tiles_f):
        block = split(fwide, t, tiles_f, deep).astype(jnp.bfloat16)
        fown[:, t * LANES : (t + 1) * LANES] = block
        fall[here, t * LANES : (t + 1) * LANES] = block
    barrier = pltpu.get_barrier_semaphore()
    for hop in range(1, n):
        pl.semaphore_signal(barrier, inc=1, device_id={"fs": (me + hop) % n}, device_id_type=MESH)
    for hop in range(1, tp):
        pl.semaphore_signal(barrier, inc=1, device_id={"tp": (mt + hop) % tp}, device_id_type=MESH)
    pl.semaphore_wait(barrier, n - 1 + tp - 1)

    def rows(ref):
        def slot(index, half):
            return ref.at[pl.ds(pl.multiple_of(index * deep + half * part, part), part)]

        return slot

    quarter = 2 * rank // tp
    far, near = (mt + 2) % tp, mt + 1 - 2 * (mt % 2)

    def quarters(index, half, which):
        return fall.at[
            pl.ds(pl.multiple_of(index * deep + half * part, part), part),
            pl.ds(pl.multiple_of(which * quarter, quarter), quarter),
        ]

    def spread(index, half, which, target, way):
        return pltpu.make_async_remote_copy(
            src_ref=quarters(index, half, which),
            dst_ref=quarters(index, half, which),
            send_sem=s_send.at[index, half, way],
            recv_sem=s_recv.at[index, half, way],
            device_id={"tp": target},
            device_id_type=MESH,
        )

    def hook(index, half):
        spread(index, half, mt, far, 0).start()
        spread(index, half, mt, near, 1).start()

    def spread_all():
        pieces = [((me + hop) % n, half) for hop in range(1, n) for half in (0, 1)]
        for index, half in pieces:
            spread(index, half, far, far, 0).wait_recv()
            spread(index, half, far, near, 2).start()
        for index, half in pieces:
            spread(index, half, near, near, 1).wait_recv()
            spread(index, half, (near + 2) % tp, near, 2).wait_recv()

    def spread_sent():
        for hop in range(1, n):
            for half in (0, 1):
                index = (me + hop) % n
                spread(index, half, mt, far, 0).wait_send()
                spread(index, half, mt, near, 1).wait_send()
                spread(index, half, far, near, 2).wait_send()

    if tp == 4 and quarter % LANES == 0:
        gather_f = Gather(n, lambda i, half: quarters(i, half, mt), f_send, f_recv, hook)
    else:
        spread_all = spread_sent = lambda: None
        gather_f = Gather(n, rows(fall), f_send, f_recv)
    gather_w = Gather(n, rows(wall), w_send, w_recv)
    gather_n = Gather(n, lambda i, half: nmall.at[i, half], n_send, n_recv)
    gather_f.begin()
    for t in range(2 * tiles_w):
        wall[here, t * LANES : (t + 1) * LANES] = split(w_ref, t, tiles_w, deep).astype(jnp.bfloat16)
    gather_w.begin()
    gather_f.turn()
    done = 1
    for head in range(heads):
        head_step(head, q_ref, k_ref, v_ref, c_ref, mix_ref, gain_ref, dq, dv)
        if done < n // 2:
            gather_f.step(done)
            done += 1
    for s in range(done, n // 2):
        gather_f.step(s)
    gather_w.turn()
    gather_f.finish_recv()
    spread_all()
    gather_w.step(1)
    for m, cot in enumerate((dq, dv)):
        reduced = jnp.dot(
            x_ref[...], fall[:, m * rank : (m + 1) * rank], preferred_element_type=jnp.float32
        ).astype(jnp.bfloat16)
        partial = lax.dot_general(
            reduced, cot[...], (((0,), (0,)), ((), ())), preferred_element_type=jnp.float32
        )
        for j in range(n):
            psend[j, m] = partial[j * rank_here : (j + 1) * rank_here].astype(psend.dtype)

    def p_copy(hop):
        peer = (me + hop) % n
        return pltpu.make_async_remote_copy(
            src_ref=psend.at[peer],
            dst_ref=precv.at[hop],
            send_sem=p_send.at[hop],
            recv_sem=p_recv.at[hop],
            device_id={"fs": peer},
            device_id_type=MESH,
        )

    for hop in range(1, n):
        p_copy(hop).start()
    for s in range(2, n // 2 - 1):
        gather_w.step(s)
    total = psend[me].astype(jnp.float32)
    for hop in range(1, n):
        p_copy(hop).wait_recv()
        total += precv[hop].astype(jnp.float32)
    length = x_ref.shape[0]
    for t in range(2 * tiles_w):
        m, lanes = t // tiles_w, slice(t % tiles_w * LANES, (t % tiles_w + 1) * LANES)
        moments = BETA * split(mom_ref, t, tiles_w, rank_here)
        moments += total[m, :, lanes] * (length * n) ** (-0.5)
        nm_ref[m, :, lanes] = moments
        nmall[me, m, :, lanes] = moments.astype(nmall.dtype)
    gather_n.begin()
    gather_w.step(n // 2 - 1)
    gather_n.turn()
    for s in range(1, n // 2):
        gather_n.step(s)
    gather_n.finish_recv()
    everything = nmall[...].astype(jnp.float32)
    squares = jnp.sum(jnp.sum(everything * everything, axis=0), axis=1)
    sums[0] = jnp.sum(squares, axis=1, keepdims=True) + jnp.zeros((2, 128), jnp.float32)

    def t_copy(hop):
        return pltpu.make_async_remote_copy(
            src_ref=sums.at[0],
            dst_ref=sums.at[hop],
            send_sem=t_send.at[hop],
            recv_sem=t_recv.at[hop],
            device_id={"tp": (mt + hop) % tp},
            device_id_type=MESH,
        )

    for hop in range(1, tp):
        t_copy(hop).start()
    gather_w.finish_recv()
    totals = sums[0]
    for hop in range(1, tp):
        t_copy(hop).wait_recv()
        totals += sums[hop]
    tot_ref[...] = totals
    for hop in range(1, tp):
        t_copy(hop).wait_send()
    for hop in range(1, n):
        p_copy(hop).wait_send()
    spread_sent()
    for gather in (gather_f, gather_w, gather_n):
        gather.finish_send()


def finish(entries, fall, wall, nmall, nm_ref, tot_ref, fown, step, nm_out, copies, wide):
    _, _, rank_here, cols = nmall.shape
    rank = fall.shape[1] // 2
    tiles = cols // LANES
    rate = RATE_BASE / jnp.sqrt(1.0 + tot_ref[...] / entries)

    def lows(rows, m):
        block = nmall[:, m].reshape(rank, cols).astype(jnp.bfloat16)
        return jnp.dot(
            rows[:, m * rank : (m + 1) * rank], block, preferred_element_type=jnp.float32
        )

    count = fall.shape[0]
    for m in range(2):
        low = lows(fall, m)
        for t in range(tiles):
            lanes = slice(t * LANES, (t + 1) * LANES)
            old = wall[:, m * cols + t * LANES : m * cols + (t + 1) * LANES].astype(jnp.float32)
            wide[pl.ds(2 * t + m, count, stride=2 * tiles), :] = (
                old - low[:, lanes] * rate[m : m + 1]
            )
    copies[...] = wide[...].astype(jnp.bfloat16)

    @pl.when(pl.program_id(0) == 0)
    def _():
        for m in range(2):
            low = lows(fown, m)
            for t in range(tiles):
                lanes = slice(t * LANES, (t + 1) * LANES)
                step[pl.ds(2 * t + m, fown.shape[0], stride=2 * tiles), :] = (
                    low[:, lanes] * rate[m : m + 1]
                )
                nm_out[pl.ds(2 * t + m, rank_here, stride=2 * tiles), :] = nm_ref[m, :, lanes]


def to_rows(array):
    rows, maps, cols = array.shape
    return array.reshape(rows, maps, cols // LANES, LANES).transpose(0, 2, 1, 3).reshape(-1, LANES)


def from_rows(array, rows):
    return (
        array.reshape(rows, -1, 2, LANES).transpose(0, 2, 1, 3).reshape(rows, 2, -1)
    )


def per_device(
    n, tp, inputs, queries, keys, values, head_cot, mixing, head_gain, factors, moments, weights
):
    length, depth = inputs.shape
    heads = mixing.shape[0]
    deep, _, rank = factors.shape
    rank_here, _, cols = moments.shape
    wire = jnp.bfloat16 if rank_here % 16 == 0 else jnp.float32
    vmem = pl.BlockSpec(memory_space=pltpu.VMEM)
    dma = pltpu.SemaphoreType.DMA
    held = pl.pallas_call(
        functools.partial(kernel, n, tp, heads),
        out_shape=(
            jax.ShapeDtypeStruct((depth, 2 * rank), jnp.bfloat16),
            jax.ShapeDtypeStruct((depth, 2 * cols), jnp.bfloat16),
            jax.ShapeDtypeStruct((n, 2, rank_here, cols), wire),
            jax.ShapeDtypeStruct((2, rank_here, cols), jnp.float32),
            jax.ShapeDtypeStruct((2, LANES), jnp.float32),
            jax.ShapeDtypeStruct((deep, 2 * rank), jnp.bfloat16),
        ),
        in_specs=[vmem] * 5 + [pl.BlockSpec(memory_space=pltpu.SMEM)] + [vmem] * 4,
        out_specs=(vmem,) * 6,
        scratch_shapes=[
            pltpu.VMEM((deep * 2 * rank // LANES, LANES), jnp.float32),
            pltpu.VMEM((length, cols), jnp.bfloat16),
            pltpu.VMEM((length, cols), jnp.bfloat16),
            pltpu.VMEM((n, 2, rank_here, cols), wire),
            pltpu.VMEM((n, 2, rank_here, cols), wire),
            pltpu.VMEM((tp, 2, LANES), jnp.float32),
            dma((n, 2, 3)), dma((n, 2)), dma((n, 2, 3)), dma((n, 2, 3)),
            dma((n, 2, 3)), dma((n, 2)),
            dma((n, 2, 3)), dma((n, 2)),
            dma((n,)), dma((n,)),
            dma((tp,)), dma((tp,)),
        ],
        compiler_params=pltpu.CompilerParams(
            collective_id=0, has_side_effects=True, vmem_limit_bytes=56 * 1024 * 1024
        ),
    )(
        inputs, queries, keys, values, head_cot, mixing, head_gain[None, :],
        to_rows(factors), to_rows(moments), to_rows(weights),
    )
    block = min(depth, 256)
    per_row = 2 * cols // LANES

    def whole(shape):
        return pl.BlockSpec(shape, lambda i: (0,) * len(shape))

    step, new_moments, copies = pl.pallas_call(
        functools.partial(finish, rank * cols * tp),
        grid=(depth // block,),
        out_shape=(
            jax.ShapeDtypeStruct((deep * per_row, LANES), jnp.float32),
            jax.ShapeDtypeStruct((rank_here * per_row, LANES), jnp.float32),
            jax.ShapeDtypeStruct((depth * per_row, LANES), jnp.bfloat16),
        ),
        in_specs=[
            pl.BlockSpec((block, 2 * rank), lambda i: (i, 0)),
            pl.BlockSpec((block, 2 * cols), lambda i: (i, 0)),
            whole((n, 2, rank_here, cols)),
            whole((2, rank_here, cols)),
            whole((2, LANES)),
            whole((deep, 2 * rank)),
        ],
        out_specs=(
            whole((deep * per_row, LANES)),
            whole((rank_here * per_row, LANES)),
            pl.BlockSpec((block * per_row, LANES), lambda i: (i, 0)),
        ),
        scratch_shapes=[pltpu.VMEM((block * per_row, LANES), jnp.float32)],
    )(*held)
    return from_rows(step, deep), from_rows(new_moments, rank_here), from_rows(copies, depth)


def solution(mesh):
    placed = (
        P("fs", None),
        P("fs", "tp"),
        P("fs", "tp"),
        P("fs", "tp"),
        P("fs", "tp"),
        P("tp"),
        P(),
        P("fs", None, None),
        P("fs", None, "tp"),
        P("fs", None, "tp"),
    )
    return jax.shard_map(
        functools.partial(per_device, mesh.shape["fs"], mesh.shape["tp"]),
        mesh=mesh,
        in_specs=placed,
        out_specs=(P("fs", None, "tp"), P("fs", None, "tp"), P(None, None, "tp")),
        check_vma=False,
    )
```

```python
import functools

import jax
import jax.numpy as jnp
from jax import lax
from jax.experimental import pallas as pl
from jax.experimental.pallas import tpu as pltpu
from jax.sharding import PartitionSpec as P

EPS = 0.05
BETA = 0.9
RATE_BASE = 0.5
MESH = pl.DeviceIdType.MESH
LANES = 128


class Gather:
    def __init__(self, n, slot, send, recv, hook=None):
        me = lax.axis_index("fs")
        self.slot, self.send, self.recv, self.hook = slot, send, recv, hook
        self.n, self.me, self.places = n, me, n // 2
        self.place, self.parity = me // 2, me % 2
        self.partner = me + 1 - 2 * self.parity
        self.started = []

    def put(self, cond, index, half, way):
        target = (self.me - 2, self.me + 2, self.partner)[way]
        if way == 0:
            cond = jnp.logical_and(cond, self.place > 0)
        elif way == 1:
            cond = jnp.logical_and(cond, self.place < self.places - 1)

        def make():
            return pltpu.make_async_remote_copy(
                src_ref=self.slot(index, half),
                dst_ref=self.slot(index, half),
                send_sem=self.send.at[index, half, way],
                recv_sem=self.recv.at[index, half],
                device_id={"fs": target},
                device_id_type=MESH,
            )

        @pl.when(cond)
        def _():
            make().start()

        self.started.append((cond, make))

    def arrive(self, cond, index, half):
        @pl.when(cond)
        def _():
            pltpu.make_async_remote_copy(
                src_ref=self.slot(index, half),
                dst_ref=self.slot(index, half),
                send_sem=self.send.at[index, half, 0],
                recv_sem=self.recv.at[index, half],
                device_id={"fs": self.partner},
                device_id_type=MESH,
            ).wait_recv()
            if self.hook is not None:
                self.hook(index, half)

    def begin(self):
        true = self.me >= 0
        for half in (0, 1):
            for way in (2, 0, 1):
                self.put(true, self.me, half, way)

    def turn(self):
        true = self.me >= 0
        self.arrive(true, self.partner, 0)
        for way in (0, 1):
            self.put(true, self.partner, 0, way)

    def step(self, s):
        for way in (1, 0):
            place = self.place - s if way == 1 else self.place + s
            cond = jnp.logical_and(place >= 0, place < self.places)
            same = 2 * place + self.parity
            other = 2 * place + 1 - self.parity
            self.arrive(cond, same, 1)
            self.put(cond, same, 1, 2)
            self.put(cond, same, 1, way)
            self.arrive(cond, same, 0)
            self.put(cond, same, 0, way)
            self.arrive(cond, other, 0)
            self.put(cond, other, 0, way)

    def finish_recv(self):
        true = self.me >= 0
        for place in range(self.places):
            self.arrive(true, 2 * place + 1 - self.parity, 1)

    def finish_send(self):
        for cond, make in self.started:

            @pl.when(cond)
            def _(make=make):
                make().wait_send()


def split(ref, t, tiles, count):
    return ref[pl.ds(t % tiles * 2 + t // tiles, count, stride=2 * tiles), :]


def head_step(head, q_ref, k_ref, v_ref, c_ref, mix_ref, gain_ref, dq_ref, dv_ref):
    length = q_ref.shape[0]
    width = gain_ref.shape[1]
    half = width // 2
    factor = half ** (-0.5)
    cols = slice(head * width, (head + 1) * width)
    query, key, value = q_ref[:, cols], k_ref[:, cols], v_ref[:, cols]
    lane = lax.broadcasted_iota(jnp.int32, (length, width), 1)
    zero = jnp.zeros_like(key)
    key0 = jnp.where(lane < half, key, zero)
    key1 = jnp.where(lane < half, zero, key)
    row = lax.broadcasted_iota(jnp.int32, (length, length), 0)
    col = lax.broadcasted_iota(jnp.int32, (length, length), 1)
    causal = col <= row
    mix = mix_ref[head]
    nt = (((1,), (1,)), ((), ()))
    tn = (((0,), (0,)), ((), ()))

    def probs(rows):
        scores = lax.dot_general(query, rows, nt, preferred_element_type=jnp.float32) * factor
        scores = jnp.where(causal, scores, -jnp.inf)
        expo = jnp.exp(scores - jnp.max(scores, axis=-1, keepdims=True))
        return expo * (1.0 / jnp.sum(expo, axis=-1, keepdims=True))

    first, second = probs(key0), probs(key1)
    mixed = (first - mix * second).astype(jnp.bfloat16)
    output = jnp.dot(mixed, value, preferred_element_type=jnp.float32)
    inverse = lax.rsqrt(jnp.mean(output * output, axis=-1, keepdims=True) + EPS)
    scaled = gain_ref[...] * c_ref[:, cols].astype(jnp.float32)
    d_out = inverse * scaled - output * (inverse * inverse * inverse) * jnp.mean(
        output * scaled, axis=-1, keepdims=True
    )
    d_out = d_out.astype(jnp.bfloat16)
    dv_ref[:, cols] = lax.dot_general(mixed, d_out, tn, preferred_element_type=jnp.float32).astype(jnp.bfloat16)
    d_mix = lax.dot_general(d_out, value, nt, preferred_element_type=jnp.float32)
    d_first = first * (d_mix - jnp.sum(first * d_mix, axis=-1, keepdims=True))
    d_second = -mix * second * (d_mix - jnp.sum(second * d_mix, axis=-1, keepdims=True))
    d_query = jnp.dot(d_first.astype(jnp.bfloat16), key0, preferred_element_type=jnp.float32)
    d_query += jnp.dot(d_second.astype(jnp.bfloat16), key1, preferred_element_type=jnp.float32)
    dq_ref[:, cols] = (d_query * factor).astype(jnp.bfloat16)


def kernel(
    n, tp, heads,
    x_ref, q_ref, k_ref, v_ref, c_ref, mix_ref, gain_ref, f_ref, mom_ref, w_ref,
    fall, wall, nmall, nm_ref, tot_ref, fown,
    fwide, dq, dv, psend, precv, sums,
    f_send, f_recv, s_send, s_recv, w_send, w_recv, n_send, n_recv, p_send, p_recv, t_send, t_recv,
):
    me = lax.axis_index("fs")
    mt = lax.axis_index("tp")
    deep = fown.shape[0]
    part = deep // 2
    cut = max(16, deep // 64 * 16)
    rank = fown.shape[1] // 2
    rank_here = rank // n
    cols = dq.shape[1]
    tiles_f, tiles_w = rank // LANES, cols // LANES
    here = pl.ds(pl.multiple_of(me * deep, deep), deep)
    fwide[...] = f_ref[...].astype(jnp.float32)
    for t in range(2 * tiles_f):
        block = split(fwide, t, tiles_f, deep).astype(jnp.bfloat16)
        fown[:, t * LANES : (t + 1) * LANES] = block
        fall[here, t * LANES : (t + 1) * LANES] = block
    barrier = pltpu.get_barrier_semaphore()
    for hop in range(1, n):
        pl.semaphore_signal(barrier, inc=1, device_id={"fs": (me + hop) % n}, device_id_type=MESH)
    for hop in range(1, tp):
        pl.semaphore_signal(barrier, inc=1, device_id={"tp": (mt + hop) % tp}, device_id_type=MESH)
    pl.semaphore_wait(barrier, n - 1 + tp - 1)

    def rows(ref):
        def slot(index, half):
            start, size = (cut, deep - cut) if half else (0, cut)
            return ref.at[pl.ds(pl.multiple_of(index * deep + start, 16), size)]

        return slot

    quarter = 2 * rank // tp
    far, near = (mt + 2) % tp, mt + 1 - 2 * (mt % 2)

    def quarters(index, half, which):
        return fall.at[
            pl.ds(pl.multiple_of(index * deep + half * part, part), part),
            pl.ds(pl.multiple_of(which * quarter, quarter), quarter),
        ]

    def spread(index, half, which, target, way):
        return pltpu.make_async_remote_copy(
            src_ref=quarters(index, half, which),
            dst_ref=quarters(index, half, which),
            send_sem=s_send.at[index, half, way],
            recv_sem=s_recv.at[index, half, way],
            device_id={"tp": target},
            device_id_type=MESH,
        )

    def hook(index, half):
        spread(index, half, mt, far, 0).start()
        spread(index, half, mt, near, 1).start()

    def spread_all():
        pieces = [((me + hop) % n, half) for hop in range(1, n) for half in (0, 1)]
        for index, half in pieces:
            spread(index, half, far, far, 0).wait_recv()
            spread(index, half, far, near, 2).start()
        for index, half in pieces:
            spread(index, half, near, near, 1).wait_recv()
            spread(index, half, (near + 2) % tp, near, 2).wait_recv()

    def spread_sent():
        for hop in range(1, n):
            for half in (0, 1):
                index = (me + hop) % n
                spread(index, half, mt, far, 0).wait_send()
                spread(index, half, mt, near, 1).wait_send()
                spread(index, half, far, near, 2).wait_send()

    if tp == 4 and quarter % LANES == 0:
        gather_f = Gather(n, lambda i, half: quarters(i, half, mt), f_send, f_recv, hook)
    else:
        spread_all = spread_sent = lambda: None
        gather_f = Gather(n, rows(fall), f_send, f_recv)
    gather_w = Gather(n, rows(wall), w_send, w_recv)
    gather_n = Gather(n, lambda i, half: nmall.at[i, half], n_send, n_recv)
    gather_f.begin()
    for t in range(2 * tiles_w):
        wall[here, t * LANES : (t + 1) * LANES] = split(w_ref, t, tiles_w, deep).astype(jnp.bfloat16)
    gather_w.begin()
    gather_f.turn()
    done = 1
    for head in range(heads):
        head_step(head, q_ref, k_ref, v_ref, c_ref, mix_ref, gain_ref, dq, dv)
        if done < n // 2:
            gather_f.step(done)
            done += 1
    for s in range(done, n // 2):
        gather_f.step(s)
    gather_w.turn()
    gather_f.finish_recv()
    spread_all()
    gather_w.step(1)
    for m, cot in enumerate((dq, dv)):
        reduced = jnp.dot(
            x_ref[...], fall[:, m * rank : (m + 1) * rank], preferred_element_type=jnp.float32
        ).astype(jnp.bfloat16)
        partial = lax.dot_general(
            reduced, cot[...], (((0,), (0,)), ((), ())), preferred_element_type=jnp.float32
        )
        for j in range(n):
            psend[j, m] = partial[j * rank_here : (j + 1) * rank_here].astype(psend.dtype)

    def p_copy(hop):
        peer = (me + hop) % n
        return pltpu.make_async_remote_copy(
            src_ref=psend.at[peer],
            dst_ref=precv.at[hop],
            send_sem=p_send.at[hop],
            recv_sem=p_recv.at[hop],
            device_id={"fs": peer},
            device_id_type=MESH,
        )

    for hop in range(1, n):
        p_copy(hop).start()
    for s in range(2, n // 2 - 1):
        gather_w.step(s)
    total = psend[me].astype(jnp.float32)
    for hop in range(1, n):
        p_copy(hop).wait_recv()
        total += precv[hop].astype(jnp.float32)
    length = x_ref.shape[0]
    for t in range(2 * tiles_w):
        m, lanes = t // tiles_w, slice(t % tiles_w * LANES, (t % tiles_w + 1) * LANES)
        moments = BETA * split(mom_ref, t, tiles_w, rank_here)
        moments += total[m, :, lanes] * (length * n) ** (-0.5)
        nm_ref[m, :, lanes] = moments
        nmall[me, m, :, lanes] = moments.astype(nmall.dtype)
    gather_n.begin()
    gather_w.step(n // 2 - 1)
    gather_n.turn()
    for s in range(1, n // 2):
        gather_n.step(s)
    gather_n.finish_recv()
    everything = nmall[...].astype(jnp.float32)
    squares = jnp.sum(jnp.sum(everything * everything, axis=0), axis=1)
    sums[0] = jnp.sum(squares, axis=1, keepdims=True) + jnp.zeros((2, 128), jnp.float32)

    def t_copy(hop):
        return pltpu.make_async_remote_copy(
            src_ref=sums.at[0],
            dst_ref=sums.at[hop],
            send_sem=t_send.at[hop],
            recv_sem=t_recv.at[hop],
            device_id={"tp": (mt + hop) % tp},
            device_id_type=MESH,
        )

    for hop in range(1, tp):
        t_copy(hop).start()
    gather_w.finish_recv()
    totals = sums[0]
    for hop in range(1, tp):
        t_copy(hop).wait_recv()
        totals += sums[hop]
    tot_ref[...] = totals
    for hop in range(1, tp):
        t_copy(hop).wait_send()
    for hop in range(1, n):
        p_copy(hop).wait_send()
    spread_sent()
    for gather in (gather_f, gather_w, gather_n):
        gather.finish_send()


def finish(entries, fall, wall, nmall, nm_ref, tot_ref, fown, step, nm_out, copies, wide):
    _, _, rank_here, cols = nmall.shape
    rank = fall.shape[1] // 2
    tiles = cols // LANES
    rate = RATE_BASE / jnp.sqrt(1.0 + tot_ref[...] / entries)

    def lows(rows, m):
        block = nmall[:, m].reshape(rank, cols).astype(jnp.bfloat16)
        return jnp.dot(
            rows[:, m * rank : (m + 1) * rank], block, preferred_element_type=jnp.float32
        )

    count = fall.shape[0]
    for m in range(2):
        low = lows(fall, m)
        for t in range(tiles):
            lanes = slice(t * LANES, (t + 1) * LANES)
            old = wall[:, m * cols + t * LANES : m * cols + (t + 1) * LANES].astype(jnp.float32)
            wide[pl.ds(2 * t + m, count, stride=2 * tiles), :] = (
                old - low[:, lanes] * rate[m : m + 1]
            )
    copies[...] = wide[...].astype(jnp.bfloat16)

    @pl.when(pl.program_id(0) == 0)
    def _():
        for m in range(2):
            low = lows(fown, m)
            for t in range(tiles):
                lanes = slice(t * LANES, (t + 1) * LANES)
                step[pl.ds(2 * t + m, fown.shape[0], stride=2 * tiles), :] = (
                    low[:, lanes] * rate[m : m + 1]
                )
                nm_out[pl.ds(2 * t + m, rank_here, stride=2 * tiles), :] = nm_ref[m, :, lanes]


def to_rows(array):
    rows, maps, cols = array.shape
    return array.reshape(rows, maps, cols // LANES, LANES).transpose(0, 2, 1, 3).reshape(-1, LANES)


def from_rows(array, rows):
    return (
        array.reshape(rows, -1, 2, LANES).transpose(0, 2, 1, 3).reshape(rows, 2, -1)
    )


def per_device(
    n, tp, inputs, queries, keys, values, head_cot, mixing, head_gain, factors, moments, weights
):
    length, depth = inputs.shape
    heads = mixing.shape[0]
    deep, _, rank = factors.shape
    rank_here, _, cols = moments.shape
    wire = jnp.bfloat16 if rank_here % 16 == 0 else jnp.float32
    vmem = pl.BlockSpec(memory_space=pltpu.VMEM)
    dma = pltpu.SemaphoreType.DMA
    held = pl.pallas_call(
        functools.partial(kernel, n, tp, heads),
        out_shape=(
            jax.ShapeDtypeStruct((depth, 2 * rank), jnp.bfloat16),
            jax.ShapeDtypeStruct((depth, 2 * cols), jnp.bfloat16),
            jax.ShapeDtypeStruct((n, 2, rank_here, cols), wire),
            jax.ShapeDtypeStruct((2, rank_here, cols), jnp.float32),
            jax.ShapeDtypeStruct((2, LANES), jnp.float32),
            jax.ShapeDtypeStruct((deep, 2 * rank), jnp.bfloat16),
        ),
        in_specs=[vmem] * 5 + [pl.BlockSpec(memory_space=pltpu.SMEM)] + [vmem] * 4,
        out_specs=(vmem,) * 6,
        scratch_shapes=[
            pltpu.VMEM((deep * 2 * rank // LANES, LANES), jnp.float32),
            pltpu.VMEM((length, cols), jnp.bfloat16),
            pltpu.VMEM((length, cols), jnp.bfloat16),
            pltpu.VMEM((n, 2, rank_here, cols), wire),
            pltpu.VMEM((n, 2, rank_here, cols), wire),
            pltpu.VMEM((tp, 2, LANES), jnp.float32),
            dma((n, 2, 3)), dma((n, 2)), dma((n, 2, 3)), dma((n, 2, 3)),
            dma((n, 2, 3)), dma((n, 2)),
            dma((n, 2, 3)), dma((n, 2)),
            dma((n,)), dma((n,)),
            dma((tp,)), dma((tp,)),
        ],
        compiler_params=pltpu.CompilerParams(
            collective_id=0, has_side_effects=True, vmem_limit_bytes=56 * 1024 * 1024
        ),
    )(
        inputs, queries, keys, values, head_cot, mixing, head_gain[None, :],
        to_rows(factors), to_rows(moments), to_rows(weights),
    )
    block = min(depth, 256)
    per_row = 2 * cols // LANES

    def whole(shape):
        return pl.BlockSpec(shape, lambda i: (0,) * len(shape))

    step, new_moments, copies = pl.pallas_call(
        functools.partial(finish, rank * cols * tp),
        grid=(depth // block,),
        out_shape=(
            jax.ShapeDtypeStruct((deep * per_row, LANES), jnp.float32),
            jax.ShapeDtypeStruct((rank_here * per_row, LANES), jnp.float32),
            jax.ShapeDtypeStruct((depth * per_row, LANES), jnp.bfloat16),
        ),
        in_specs=[
            pl.BlockSpec((block, 2 * rank), lambda i: (i, 0)),
            pl.BlockSpec((block, 2 * cols), lambda i: (i, 0)),
            whole((n, 2, rank_here, cols)),
            whole((2, rank_here, cols)),
            whole((2, LANES)),
            whole((deep, 2 * rank)),
        ],
        out_specs=(
            whole((deep * per_row, LANES)),
            whole((rank_here * per_row, LANES)),
            pl.BlockSpec((block * per_row, LANES), lambda i: (i, 0)),
        ),
        scratch_shapes=[pltpu.VMEM((block * per_row, LANES), jnp.float32)],
    )(*held)
    return from_rows(step, deep), from_rows(new_moments, rank_here), from_rows(copies, depth)


def solution(mesh):
    placed = (
        P("fs", None),
        P("fs", "tp"),
        P("fs", "tp"),
        P("fs", "tp"),
        P("fs", "tp"),
        P("tp"),
        P(),
        P("fs", None, None),
        P("fs", None, "tp"),
        P("fs", None, "tp"),
    )
    return jax.shard_map(
        functools.partial(per_device, mesh.shape["fs"], mesh.shape["tp"]),
        mesh=mesh,
        in_specs=placed,
        out_specs=(P("fs", None, "tp"), P("fs", None, "tp"), P(None, None, "tp")),
        check_vma=False,
    )
```
